256 devices in a mesh: sp: 32 (over z, y), tp: 8 (over x, core).
Axes of the slice: x: 4, y: 4, z: 8, core: 2. Of those that a mesh axis runs over, the one named last changes fastest.
Arguments:
- tokens: bfloat16 [16384, 4096], P('sp', 'tp'), may hold values from -64 to 64
- norm_gain: float32 [4096], replicated, may hold values from 0.1 to 1.9
- w_query: bfloat16 [4096, 1024], P(None, 'tp'), may hold values from -0.09375 to 0.09375
- w_key: bfloat16 [4096, 1024], P(None, 'tp'), may hold values from -0.09375 to 0.09375
- w_value: bfloat16 [4096, 1024], P(None, 'tp'), may hold values from -0.09375 to 0.09375
- w_gate_out: bfloat16 [4096, 1024], P(None, 'tp'), may hold values from -0.09375 to 0.09375
- w_gate_in: bfloat16 [4096, 1024], P(None, 'tp'), may hold values from -0.09375 to 0.09375
- w_conv_in: bfloat16 [4096, 1024], P(None, 'tp'), may hold values from -0.09375 to 0.09375
- conv_taps: float32 [3, 1024], replicated, may hold values from -3.5 to 3.5
- key_bias: bfloat16 [16384, 16], P('sp', 'tp'), may hold values from -16 to 0
- mix_gain: float32 [2048], replicated, may hold values from 0.1 to 1.9
- out_attn: bfloat16 [1024, 4096], P('tp'), may hold values from -0.125 to 0.125
- out_conv: bfloat16 [1024, 4096], P('tp'), may hold values from -0.125 to 0.125
Outputs:
- mixed: bfloat16 [16384, 4096], P('sp', 'tp')
The draws below stay inside these ranges and needn't reach their ends.
All inputs are finite; a program needn't handle non-finite values.
Results may differ from the reference program's by a relative error of at most 0.015.
Values may be sent and summed in bfloat16 or wider, within the bound.
No kernel may reach another device: no remote copies, remote signals or barrier semaphores. Data moves between devices by JAX's collectives and lax.ppermute only.
A program may use at most 128 MiB of HBM per device.

```python
import math
import jax
import jax.numpy as jnp
from jax import lax

D = 4096
HEAD = 64
STICK_HEADS = 16
CONV_CH = 1024
CONV_WIDTH = 3
TOK_DEV = 512
SEQUENCE_LENGTH = 16384
N_SP = 32


def draw_tokens(key, part):
    key_matrix = jax.random.split(key, 3)
    base = jax.random.normal(key_matrix[0], (SEQUENCE_LENGTH, D), jnp.float32)
    ramp = jnp.exp(jnp.log(3.0) * jnp.arange(D, dtype=jnp.float32) / D)
    rough = jnp.exp(jax.random.uniform(key_matrix[1], (D,), jnp.float32, 0.0, jnp.log(10.0)))
    row_scale = jnp.exp(jax.random.uniform(key_matrix[2], (SEQUENCE_LENGTH, 1), jnp.float32, -1.0, 1.0))
    value_matrix = base * ramp * rough * row_scale / 3.0
    return jnp.clip(value_matrix, -64.0, 64.0).astype(jnp.bfloat16)


def draw_key_bias(key, part):
    key_matrix = jax.random.split(key, 7)
    fast_share = 0.5
    slow_lo = 0.1
    slow_hi = 1.4
    is_fast = jax.random.uniform(key_matrix[0], (STICK_HEADS,), jnp.float32) < fast_share
    fast_level = jax.random.uniform(key_matrix[1], (STICK_HEADS,), jnp.float32, -5.0, -3.5)
    slow_rate = jnp.exp(jax.random.uniform(key_matrix[2], (STICK_HEADS,), jnp.float32, jnp.log(slow_lo), jnp.log(slow_hi)))
    slow_level = jnp.log(slow_rate / SEQUENCE_LENGTH)
    level = jnp.where(is_fast, fast_level, slow_level)
    block_count = SEQUENCE_LENGTH // TOK_DEV
    shifts = jax.random.uniform(key_matrix[3], (block_count,), jnp.float32, -0.8, 0.8)
    per_position = jnp.repeat(shifts, TOK_DEV)
    rough = jnp.clip(0.5 * jax.random.normal(key_matrix[4], (SEQUENCE_LENGTH, STICK_HEADS), jnp.float32), -1.5, 1.5)
    spike_position = jax.random.randint(key_matrix[5], (4, STICK_HEADS), 0, SEQUENCE_LENGTH)
    match_count = jnp.any(jnp.arange(SEQUENCE_LENGTH, dtype=jnp.int32)[:, None, None] == spike_position[None], axis=1)
    portion_fraction = jax.random.uniform(key_matrix[6], (SEQUENCE_LENGTH, STICK_HEADS), jnp.float32, 0.2, 0.5)
    spike_tokens = jnp.log(portion_fraction) - jnp.log1p(-portion_fraction)
    value_matrix = level[None, :] + per_position[:, None] + rough
    return jnp.where(match_count, spike_tokens, value_matrix).astype(jnp.bfloat16)


def block_levels(rng, shape, cuts, least, top_value):
    level, own = 1.0, jax.random.fold_in(rng, 6)
    for dim, parts in cuts:
        steps = jnp.exp(jax.random.uniform(jax.random.fold_in(own, dim), (parts,), jnp.float32, least / len(cuts), top_value / len(cuts)))
        level = level * jnp.repeat(steps, shape[dim] // parts).reshape([-1 if axis == dim else 1 for axis in range(len(shape))])
    return level


def centred(own_key, dims, scale, bound, cuts=(), kind=jnp.bfloat16):
    factor_of = block_levels(own_key, dims, cuts, -0.22, 0.18) if cuts else 1.0
    values = jax.random.normal(own_key, dims, jnp.float32) * scale * factor_of
    return jnp.minimum(jnp.maximum(values, -bound), bound).astype(kind)


def setup_inputs(seed: int = 0) -> dict:
    streams_of = jax.random.split(jax.random.key(seed), 14)
    return {
        "tokens": draw_tokens(jax.random.fold_in(streams_of[13], 71), 0),
        "norm_gain": jnp.clip(1.0 + 0.18 * jax.random.normal(streams_of[1], (D,), jnp.float32), 0.1, 1.9),
        "w_query": centred(streams_of[2], (D, STICK_HEADS * HEAD), D ** -0.5, 0.09375, ((1, 8),)),
        "w_key": centred(streams_of[3], (D, STICK_HEADS * HEAD), D ** -0.5, 0.09375, ((1, 8),)),
        "w_value": centred(streams_of[4], (D, STICK_HEADS * HEAD), D ** -0.5, 0.09375, ((1, 8),)),
        "w_gate_out": centred(streams_of[5], (D, CONV_CH), D ** -0.5, 0.09375, ((1, 8),)),
        "w_gate_in": centred(streams_of[6], (D, CONV_CH), D ** -0.5, 0.09375, ((1, 8),)),
        "w_conv_in": centred(streams_of[7], (D, CONV_CH), D ** -0.5, 0.09375, ((1, 8),)),
        "conv_taps": centred(streams_of[8], (CONV_WIDTH, CONV_CH), CONV_WIDTH ** -0.5, 3.5, (), jnp.float32),
        "key_bias": draw_key_bias(jax.random.fold_in(streams_of[13], 71), 0),
        "mix_gain": jnp.clip(1.0 + 0.18 * jax.random.normal(streams_of[10], (STICK_HEADS * HEAD + CONV_CH,), jnp.float32), 0.1, 1.9),
        "out_attn": centred(streams_of[11], (STICK_HEADS * HEAD, D), (STICK_HEADS * HEAD + CONV_CH) ** -0.5, 0.125, ((0, 8),)),
        "out_conv": centred(streams_of[12], (CONV_CH, D), (STICK_HEADS * HEAD + CONV_CH) ** -0.5, 0.125, ((0, 8),)),
    }


eps = 1e-06

def stick_terms(queries, key_rows, value_rows, bias_rows, survival, causal):
    tok_rows, head_count, head_width = queries.shape
    key_count = key_rows.shape[0]
    key_span = math.gcd(key_count, 128)
    blocks = key_count // key_span
    key_heads = key_rows.reshape(key_count, head_count, head_width)
    value_heads = value_rows.reshape(key_count, head_count, head_width)
    scores = jnp.einsum('qhe,khe->hqk', queries.astype(jnp.float32), key_heads.astype(jnp.float32))
    scores = scores * head_width ** (-0.5) + jnp.transpose(bias_rows.astype(jnp.float32))[:, None, :]
    log_rest = jax.nn.log_sigmoid(-scores)
    log_take = jax.nn.log_sigmoid(scores)
    earlier = jnp.arange(key_count)[None, :] < jnp.arange(tok_rows)[:, None]
    if causal:
        log_rest = jnp.where(earlier[None], log_rest, 0.0)
    pieces = log_rest.reshape(head_count, tok_rows, blocks, key_span)
    inner = jnp.arange(key_span)
    after_mat = (inner[:, None] > inner[None, :]).astype(jnp.float32)
    within = jnp.einsum('hqbj,js->hqbs', pieces, after_mat, precision=lax.Precision.HIGHEST)
    totals = lax.optimization_barrier(jnp.sum(pieces, axis=-1))
    outer = jnp.arange(blocks)
    later_mat = (outer[:, None] > outer[None, :]).astype(jnp.float32)
    later_sum = jnp.einsum('hqb,bc->hqc', totals, later_mat, precision=lax.Precision.HIGHEST)
    after_sum = within + later_sum[..., None] + survival[:, :, None, None]
    weights = jnp.exp(log_take + after_sum.reshape(head_count, tok_rows, key_count))
    if causal:
        weights = jnp.where(earlier[None], weights, 0.0)
    weights = lax.optimization_barrier(weights.astype(jnp.bfloat16)).astype(jnp.float32)
    result = jnp.einsum('hqk,khe->qhe', weights, value_heads.astype(jnp.float32))
    return (result, survival + lax.optimization_barrier(jnp.sum(totals, axis=-1)))

def group_norm(value_matrix, gain):
    tok_rows = value_matrix.shape[0]
    grouped = value_matrix.reshape(tok_rows, -1, HEAD)
    grouped = grouped * lax.rsqrt(lax.optimization_barrier(jnp.mean(grouped * grouped, axis=-1, keepdims=True)) + eps)
    return grouped.reshape(tok_rows, -1) * gain

def reference(tokens, norm_gain, w_query, w_key, w_value, w_gate_out, w_gate_in, w_conv_in, conv_taps, key_bias, mix_gain, out_attn, out_conv):
    tok_float = tokens.astype(jnp.float32)
    row_scale = lax.rsqrt(lax.optimization_barrier(jnp.mean(tok_float * tok_float, axis=1, keepdims=True)) + eps)
    normed = (tok_float * row_scale * norm_gain).astype(jnp.bfloat16)

    def project(weight):
        return lax.optimization_barrier(jnp.dot(normed, weight, preferred_element_type=jnp.float32).astype(jnp.bfloat16))
    queries = project(w_query).reshape(SEQUENCE_LENGTH, STICK_HEADS, HEAD)
    key_rows = project(w_key)
    value_rows = project(w_value)
    zero_state = jnp.zeros((STICK_HEADS, TOK_DEV), jnp.float32)

    def attend_block(block_index):
        block_start = block_index * TOK_DEV
        own_queries = lax.dynamic_slice_in_dim(queries, block_start, TOK_DEV, 0)
        own_keys = lax.dynamic_slice_in_dim(key_rows, block_start, TOK_DEV, 0)
        own_values = lax.dynamic_slice_in_dim(value_rows, block_start, TOK_DEV, 0)
        own_bias = lax.dynamic_slice_in_dim(key_bias, block_start, TOK_DEV, 0)
        result, survival = stick_terms(own_queries, own_keys, own_values, own_bias, zero_state, True)

        def further(offset, loop_state):
            running, carried = loop_state
            key_start = (block_index - offset) * TOK_DEV
            far_keys = lax.dynamic_slice_in_dim(key_rows, key_start, TOK_DEV, 0)
            far_values = lax.dynamic_slice_in_dim(value_rows, key_start, TOK_DEV, 0)
            far_bias = lax.dynamic_slice_in_dim(key_bias, key_start, TOK_DEV, 0)
            added, carried = stick_terms(own_queries, far_keys, far_values, far_bias, carried, False)
            return (running + added, carried)
        result, survival = lax.fori_loop(jnp.int32(1), block_index + 1, further, (result, survival))
        return result
    attended = lax.map(attend_block, jnp.arange(N_SP, dtype=jnp.int32))
    attended = attended.reshape(SEQUENCE_LENGTH, STICK_HEADS * HEAD)
    gate_out = project(w_gate_out).astype(jnp.float32)
    mixed_in = project(w_gate_in).astype(jnp.float32) * project(w_conv_in).astype(jnp.float32)
    padded = jnp.pad(mixed_in, ((CONV_WIDTH - 1, 0), (0, 0)))
    convolved = jnp.zeros((SEQUENCE_LENGTH, CONV_CH), jnp.float32)
    for tap_index in range(CONV_WIDTH):
        convolved = convolved + conv_taps[tap_index] * padded[tap_index:tap_index + SEQUENCE_LENGTH]
    conv_out = gate_out * convolved
    attn_normed = group_norm(attended, mix_gain[:STICK_HEADS * HEAD]).astype(jnp.bfloat16)
    conv_normed = group_norm(conv_out, mix_gain[STICK_HEADS * HEAD:]).astype(jnp.bfloat16)
    total = jnp.dot(attn_normed, out_attn, preferred_element_type=jnp.float32)
    total = total + jnp.dot(conv_normed, out_conv, preferred_element_type=jnp.float32)
    return total.astype(jnp.bfloat16)
```

```python
import functools

import jax
import numpy as np
import jax.numpy as jnp
from jax import lax
from jax.experimental import pallas as pl
from jax.experimental.pallas import tpu as pltpu
from jax.sharding import PartitionSpec as P

HEAD = 64
STICK_HEADS = 16
CONV_WIDTH = 3
FEATURES = 4096
NY = 4
EPS = 1e-06


LOG2E = 1.4426950408889634
KT = 256
ROWS = 512
UN = 2
QC = 512
L1, L2, L3 = 1, 1, 1
QS = 1
f32, bf16 = jnp.float32, jnp.bfloat16


def bf16_parts(value, count):
    parts = []
    for _ in range(count):
        part = float(np.float32(value).astype(jnp.bfloat16))
        parts.append(part)
        value -= part
    return parts


def prep_kernel(zy, *refs):
    kv, bias, kaug, vt = refs[:4], refs[4:8], refs[8], refs[9]
    lane = lax.broadcasted_iota(jnp.int32, (ROWS, 128), 1)
    low = lane < 64
    for i in range(4):
        at = pl.multiple_of(lax.rem(zy[1] - i + 4, 4) * ROWS, ROWS)
        k = kv[i][:, :128].astype(f32)
        turned = pltpu.roll(k, 64, 1)
        b = bias[i][...].astype(f32)
        for h in range(2):
            both = jnp.where(low, k, turned) if h == 0 else jnp.where(low, turned, k)
            kaug[h, pl.ds(at, ROWS), :128] = both.astype(bf16)
            col = jnp.broadcast_to(b[:, h : h + 1], (ROWS, 128))
            kaug[h, pl.ds(at, ROWS), 128:] = jnp.where(lane < 3, col, 0.0).astype(bf16)
        vt[:, pl.ds(at, ROWS)] = kv[i][:, 128:].astype(f32).T.astype(bf16)


def attn_kernel(steps, nz, zy, *refs):
    n = len(steps)
    qrefs, kaug, vt = refs[:n], refs[n], refs[n + 1]
    outs = refs[n + 2 : 2 * n + 2]
    qa, r, s, after = refs[2 * n + 2 :]
    after[...] = jnp.where(
        lax.broadcasted_iota(jnp.int32, (KT, KT), 1) > lax.broadcasted_iota(jnp.int32, (KT, KT), 0), -1.0, 0.0
    ).astype(bf16)

    def tiles(js, own):
        units = [(j, h, q) for j in js for q in range(ROWS // QC) for h in range(2)]
        n = len(units)
        carry = {(h, q): s[8 * h : 8 * h + 1, q * QC : q * QC + QC] for h in range(2) for q in range(ROWS // QC)}
        zs, takes, sums, sps, outs_ = {}, {}, {}, {}, {}

        def score(u):
            j, h, q = units[u]
            at = pl.multiple_of(j * KT, KT)
            zs[u] = jnp.dot(kaug[h, pl.ds(at, KT), :], qa[h, :, q * QC : q * QC + QC], preferred_element_type=f32)

        def soft(u):
            j, h, q = units[u]
            z = zs.pop(u)
            sp = jnp.maximum(z, lax.log2(1.0 + jnp.exp2(jnp.minimum(z, 126.0))))
            take = z - sp
            if own is not None:
                ok = (
                    lax.broadcasted_iota(jnp.int32, (KT, QC), 0) + own * KT
                    < lax.broadcasted_iota(jnp.int32, (KT, QC), 1) + q * QC
                )
                sp = jnp.where(ok, sp, 0.0)
                take = jnp.where(ok, take, -1e30)
            takes[u], sps[u] = take, sp[0:1, :]
            sums[u] = jnp.dot(after[...], sp.astype(bf16), preferred_element_type=f32)

        def weigh(u):
            j, h, q = units[u]
            at = pl.multiple_of(j * KT, KT)
            a = sums.pop(u)
            w = jnp.exp2(takes.pop(u) + a).astype(bf16)
            outs_[u] = (
                jnp.dot(vt[64 * h : 64 * h + 64, pl.ds(at, KT)], w, preferred_element_type=f32),
                jnp.exp2(carry[h, q]),
            )
            carry[h, q] = carry[h, q] + (a[0:1, :] - sps.pop(u))

        def add(u):
            j, h, q = units[u]
            o, scale = outs_.pop(u)
            r[64 * h : 64 * h + 64, q * QC : q * QC + QC] += scale * o

        stages = (score, soft, weigh, add)
        lags = (0, L1, L1 + L2, L1 + L2 + L3)
        for t in range(n + lags[-1]):
            for stage, lag in zip(stages, lags):
                if 0 <= t - lag < n:
                    stage(t - lag)
        for (h, q), value in carry.items():
            s[8 * h : 8 * h + 1, q * QC : q * QC + QC] = value

    c = bf16_parts(LOG2E, 3)
    for i, k in enumerate(steps):

        def step(i=i, k=k):
            q = (qrefs[i][...].astype(f32) * (LOG2E / 8)).T
            hi = q.astype(bf16).astype(f32)
            lo = q - hi
            row = lax.broadcasted_iota(jnp.int32, (128, ROWS), 0)
            tail = jnp.where(row == 0, c[0], jnp.where(row == 1, c[1], jnp.where(row == 2, c[2], 0.0))).astype(bf16)
            for h in range(2):
                mine = slice(64 * h, 64 * h + 64)
                qa[h, :64, :] = hi[mine].astype(bf16)
                qa[h, 64:128, :] = lo[mine].astype(bf16)
                qa[h, 128:, :] = tail
            r[...] = jnp.zeros_like(r)
            s[...] = jnp.zeros_like(s)
            if k == 0:
                y = zy[1]
                tiles([2 * y + 1], 1)
                tiles([2 * y], 0)

                @pl.loop(0, y)
                def _(m):
                    tiles([2 * (y - 1 - m) + 1, 2 * (y - 1 - m)], None)
            else:

                @pl.loop(0, 8 // UN)
                def _(m):
                    tiles([7 - UN * m - u for u in range(UN)], None)

            outs[i][:128, :] = r[...].astype(bf16)
            rows16 = lax.broadcasted_iota(jnp.int32, (16, ROWS), 0)
            block = jnp.zeros((16, ROWS), f32)
            for h in range(2):
                line = s[8 * h : 8 * h + 1, :]
                big = line.astype(bf16).astype(f32)
                for p, part in enumerate((big, line - big)):
                    block = jnp.where(rows16 == h * 2 + p, jnp.broadcast_to(part, (16, ROWS)), block)
            outs[i][128:, :] = block.astype(bf16)

        if k == 0:
            step()
        else:
            pl.when(zy[0] + k <= nz - 1)(step)


def combine_kernel(nk, gain, *refs):
    payloads, out = refs[:nk], refs[nk]
    heads = []
    for h in range(2):
        mine = slice(64 * h, 64 * h + 64)
        total = payloads[0][mine, :].astype(f32)
        s = jnp.zeros((1, ROWS), f32)
        for k in range(1, nk):
            b = payloads[k - 1][128:, :].astype(f32)
            s = s + b[2 * h : 2 * h + 1] + b[2 * h + 1 : 2 * h + 2]
            total = total + jnp.exp2(s) * payloads[k][mine, :].astype(f32)
        mean = jnp.sum(total * total, axis=0, keepdims=True) * (1.0 / 64)
        heads.append(total * lax.rsqrt(mean + 1e-6))
    out[...] = (jnp.concatenate(heads, axis=0).T * gain[...]).astype(bf16)


VM = pl.BlockSpec(memory_space=pltpu.VMEM)
SM = pl.BlockSpec(memory_space=pltpu.SMEM)
PARAMS = pltpu.CompilerParams(vmem_limit_bytes=48 * 1024 * 1024)


def prep(zy, kvs, biases):
    return pl.pallas_call(
        prep_kernel,
        out_shape=(jax.ShapeDtypeStruct((2, 2048, 256), bf16), jax.ShapeDtypeStruct((128, 2048), bf16)),
        in_specs=[SM] + [VM] * 8,
        out_specs=(VM, VM),
        compiler_params=PARAMS,
        name="prep",
    )(zy, *kvs, *biases)


def attend(steps, nz, zy, qs, kaug, vt):
    n = len(steps)
    cost = pl.CostEstimate(flops=2 * n * ROWS * 2048 * 256 * 6, bytes_accessed=4 * 2**20, transcendentals=3 * n * ROWS * 2048 * 2)
    return pl.pallas_call(
        functools.partial(attn_kernel, steps, nz),
        out_shape=tuple(jax.ShapeDtypeStruct((144, ROWS), bf16) for _ in steps),
        in_specs=[SM] + [VM] * (n + 2),
        out_specs=tuple(VM for _ in steps),
        scratch_shapes=[
            pltpu.VMEM((2, 256, ROWS), bf16),
            pltpu.VMEM((128, ROWS), f32),
            pltpu.VMEM((16, ROWS), f32),
            pltpu.VMEM((KT, KT), bf16),
        ],
        cost_estimate=cost,
        compiler_params=PARAMS,
        name="attend_" + "_".join(map(str, steps)),
    )(zy, *qs, kaug, vt)


def combine(gain, payloads):
    n = len(payloads)
    return pl.pallas_call(
        functools.partial(combine_kernel, n),
        out_shape=jax.ShapeDtypeStruct((ROWS, 128), bf16),
        in_specs=[VM] * (n + 1),
        out_specs=VM,
        compiler_params=PARAMS,
        name="combine",
    )(gain, *payloads)


def project_kernel(count, first, last, ids, gains, *refs):
    parts, refs = refs[: 2 * count], refs[2 * count :]
    weights, refs = refs[:6], refs[6:]
    if not first:
        before, refs = refs[:2], refs[2:]
    if last:
        outs, (acc, ssq) = refs[:3], refs[3:]
    else:
        acc, ssq = refs
    g = pl.program_id(0)

    @pl.when(g == 0)
    def _():
        if first:
            acc[...] = jnp.zeros_like(acc)
            ssq[...] = jnp.zeros_like(ssq)
        else:
            acc[...] = before[0][...]
            ssq[...] = before[1][...]

    w = jnp.concatenate([r[...] for r in weights], axis=1)
    for i in range(count):

        @pl.when(g == i)
        def _(i=i):
            for half in range(2):
                rows = slice(half * 256, half * 256 + 256)
                x = parts[2 * i + half][...].astype(f32)
                sq = x * x
                ssq[rows, :] += sq[:, :128] + sq[:, 128:256] + sq[:, 256:384] + sq[:, 384:]
                acc[rows, :] += jnp.dot((x * gains[...][0]).astype(bf16), w, preferred_element_type=f32)

    if last:

        @pl.when(g == count - 1)
        def _():
            mean = jnp.sum(ssq[...], axis=1, keepdims=True) * (1.0 / FEATURES)
            res = (acc[...] * lax.rsqrt(mean + EPS)).astype(bf16)
            outs[0][...] = res[:, :128]
            outs[1][...] = res[:, 128:384]
            outs[2][...] = res[:, 384:]


def project(ids, parts, gains, weights, before, last):
    count = len(parts)
    flat, specs = [], []
    for top, bottom in parts:
        for piece in (top, bottom):
            array, at = piece
            flat.append(array)
            specs.append(pl.BlockSpec((256, 512), lambda g, ids, at=at: (at, 0)))
    wspec = pl.BlockSpec((512, 128), lambda g, ids: (ids[g], 0))
    whole = lambda shape: pl.BlockSpec(shape, lambda g, ids: (0, 0))
    state = (jax.ShapeDtypeStruct((ROWS, 768), f32), jax.ShapeDtypeStruct((ROWS, 128), f32))
    shapes = state
    if last:
        shapes = tuple(jax.ShapeDtypeStruct((ROWS, n), bf16) for n in (128, 256, 384))
    extra = () if before is None else before
    return pl.pallas_call(
        functools.partial(project_kernel, count, before is None, last),
        grid_spec=pltpu.PrefetchScalarGridSpec(
            num_scalar_prefetch=1,
            grid=(count,),
            in_specs=[pl.BlockSpec((1, 1, 512), lambda g, ids: (ids[g], 0, 0))]
            + specs
            + [wspec] * 6
            + [whole(a.shape) for a in extra],
            out_specs=tuple(whole(s.shape) for s in shapes),
            scratch_shapes=[pltpu.VMEM(s.shape, f32) for s in state] if last else [],
        ),
        out_shape=shapes,
        cost_estimate=pl.CostEstimate(flops=2 * count * 512 * 512 * 768, bytes_accessed=count * 2**20, transcendentals=0),
        compiler_params=PARAMS,
        name="project_%d" % count,
    )(ids, gains, *flat, *weights, *extra)


def output_kernel(ids, w, *refs):
    parts, out = refs[:-1], refs[-1]
    for half in range(2):
        rows = slice(half * 256, half * 256 + 256)
        total = jnp.zeros((256, 512), f32)
        for i in range(8):
            total = total + jnp.dot(parts[2 * i + half][...], w[ids[i]], preferred_element_type=f32)
        out[rows, :] = total.astype(bf16)


def output(ids, w, parts):
    flat, specs = [], []
    for pair in parts:
        for array, at in pair:
            flat.append(array)
            specs.append(pl.BlockSpec((256, 256), lambda g, at=at: (at, 0)))
    return pl.pallas_call(
        output_kernel,
        grid=(1,),
        in_specs=[SM, pl.BlockSpec((8, 256, 512), lambda g: (0, 0, 0))] + specs,
        out_specs=pl.BlockSpec((ROWS, 512), lambda g: (0, 0)),
        out_shape=jax.ShapeDtypeStruct((ROWS, 512), bf16),
        cost_estimate=pl.CostEstimate(flops=2 * 512 * 2048 * 512, bytes_accessed=4 * 2**20, transcendentals=0),
        compiler_params=PARAMS,
        name="output",
    )(ids, w, *flat)


def along_x(shard, by):
    return lax.ppermute(shard, "tp", [(i, (i + 2 * by) % 8) for i in range(8)])


def other_core(shard):
    return lax.ppermute(shard, "tp", [(i, i ^ 1) for i in range(8)])


def along_y(shard, by):
    count = lax.axis_size("sp")
    return lax.ppermute(shard, "sp", [(i, i // NY * NY + (i + by) % NY) for i in range(count)])


def along_z(shard, by):
    count = lax.axis_size("sp")
    return lax.ppermute(shard, "sp", [(i, i + NY * by) for i in range(count) if 0 <= i + NY * by < count])


def whole(array):
    return ((array, 0), (array, 1))


def share(own):
    half = own.shape[0] // 2
    own_s = other_core(own)
    a, b = along_x(own, 1), along_x(own, -1)
    top, bottom = along_x(a[:half], 1), along_x(b[half:], -1)
    a_s, b_s = other_core(a), other_core(b)
    top_s, bottom_s = other_core(top), other_core(bottom)
    return (
        [whole(own), whole(own_s)],
        [whole(a), whole(a_s), whole(b), whole(b_s)],
        [((top, 0), (bottom, 0)), ((top_s, 0), (bottom_s, 0))],
    )


def share_ids(t):
    s = t ^ 1
    return jnp.stack([t, s, (t + 6) % 8, (s + 6) % 8, (t + 2) % 8, (s + 2) % 8, (t + 4) % 8, (s + 4) % 8]).astype(jnp.int32)


def group_norm(value_matrix, gain):
    tok_rows = value_matrix.shape[0]
    grouped = value_matrix.reshape(tok_rows, -1, HEAD)
    grouped = grouped * lax.rsqrt(jnp.mean(grouped * grouped, axis=-1, keepdims=True) + EPS)
    return grouped.reshape(tok_rows, -1) * gain


def per_device(
    tokens,
    norm_gain,
    w_query,
    w_key,
    w_value,
    w_gate_out,
    w_gate_in,
    w_conv_in,
    conv_taps,
    key_bias,
    mix_gain,
    out_attn,
    out_conv,
):
    tok_rows = tokens.shape[0]
    cols = w_query.shape[1]
    tp_index = lax.axis_index("tp")
    sp_index = lax.axis_index("sp")
    nz = lax.axis_size("sp") // NY
    zy = jnp.stack([sp_index // NY, sp_index % NY]).astype(jnp.int32)
    ids = share_ids(tp_index)
    weights = (w_query, w_key, w_value, w_gate_out, w_gate_in, w_conv_in)
    gains = norm_gain.reshape(8, 1, 512)

    near, mid, far = share(tokens)
    bias = jnp.pad(key_bias, ((0, 0), (0, 126)))
    biases = [bias] + [along_y(bias, k) for k in range(1, NY)]
    state = project(ids[:2], near, gains, weights, None, False)
    state = project(ids[2:6], mid, gains, weights, state, False)
    queries, keys_values, gates = project(ids[6:], far, gains, weights, state, True)

    qs = [queries] + [along_z(queries, -k) for k in range(1, nz)]
    kvs = [keys_values] + [along_y(keys_values, k) for k in range(1, NY)]

    out_rows = jnp.concatenate([out_attn, out_conv], axis=0)
    out_rows = out_rows.reshape(2 * cols, 8, 512).transpose(1, 0, 2)
    out_rows = lax.optimization_barrier((out_rows, queries))[0]
    out_cols = lax.all_to_all(out_rows, "tp", 0, 0, tiled=True)

    edge = CONV_WIDTH - 1
    count = lax.axis_size("sp")
    before = lax.ppermute(gates[tok_rows - edge :, cols:], "sp", [(i, i + 1) for i in range(count - 1)])
    pair = jnp.concatenate([before, gates[:, cols:]], axis=0).astype(f32)
    padded = pair[:, :cols] * pair[:, cols:]
    own_taps = lax.dynamic_slice_in_dim(conv_taps, tp_index * cols, cols, 1)
    convolved = jnp.zeros((tok_rows, cols), f32)
    for tap_index in range(CONV_WIDTH):
        convolved = convolved + own_taps[tap_index] * padded[tap_index : tap_index + tok_rows]
    conv_out = gates[:, :cols].astype(f32) * convolved
    attn_gain = lax.dynamic_slice_in_dim(mix_gain, tp_index * cols, cols)
    conv_gain = lax.dynamic_slice_in_dim(mix_gain, STICK_HEADS * HEAD + tp_index * cols, cols)
    conv_normed = group_norm(conv_out, conv_gain).astype(bf16)

    kaug, vcat = prep(zy, kvs, biases)
    payloads = []
    for k in range(nz):
        (mine,) = attend((k,), nz, zy, [qs[k]], kaug, vcat)
        payloads.append(along_z(mine, k) if k else mine)
    attn_normed = combine(attn_gain[None], payloads)
    near, mid, far = share(jnp.concatenate([attn_normed, conv_normed], axis=1))
    return output(ids, out_cols, near + mid + far)


def solution(mesh):
    in_specs = (
        P("sp", "tp"),
        P(),
        P(None, "tp"),
        P(None, "tp"),
        P(None, "tp"),
        P(None, "tp"),
        P(None, "tp"),
        P(None, "tp"),
        P(),
        P("sp", "tp"),
        P(),
        P("tp", None),
        P("tp", None),
    )
    return jax.shard_map(
        per_device, mesh=mesh, in_specs=in_specs, out_specs=P("sp", "tp"), check_vma=False
    )
```

```python
import functools

import jax
import numpy as np
import jax.numpy as jnp
from jax import lax
from jax.experimental import pallas as pl
from jax.experimental.pallas import tpu as pltpu
from jax.sharding import PartitionSpec as P

HEAD = 64
STICK_HEADS = 16
CONV_WIDTH = 3
FEATURES = 4096
NY = 4
CHIP, CORE, ZAT, YAT = 8, 9, 10, 11
GROUPS = ((7, 6, 5, 4), (3, 2, 1), (0,))
EPS = 1e-06


LOG2E = 1.4426950408889634
KT = 256
ROWS = 512
UN = 4
QC = 256
L1, L2, L3 = 2, 1, 1
QS = 1
f32, bf16 = jnp.float32, jnp.bfloat16


def bf16_parts(value, count):
    parts = []
    for _ in range(count):
        part = float(np.float32(value).astype(jnp.bfloat16))
        parts.append(part)
        value -= part
    return parts


def prep_kernel(zy, *refs):
    kv, kaug, vt = refs[:4], refs[4], refs[5]
    low = lax.broadcasted_iota(jnp.int32, (ROWS, 128), 1) < 64
    row = lax.broadcasted_iota(jnp.int32, (128, ROWS), 0)
    for i in range(4):
        at = pl.multiple_of(lax.rem(zy[YAT] - i + 4, 4) * ROWS, ROWS)
        k = kv[i][:ROWS, :128].astype(f32)
        turned = pltpu.roll(k, 64, 1)
        b = kv[i][ROWS:, :].astype(f32)
        for h in range(2):
            both = jnp.where(low, k, turned) if h == 0 else jnp.where(low, turned, k)
            kaug[h, pl.ds(at, ROWS), :128] = both.astype(bf16)
            line = jnp.concatenate([b[2 * h : 2 * h + 1], b[2 * h + 1 : 2 * h + 2]], axis=1)
            tail = jnp.where(row < 3, jnp.broadcast_to(line, (128, ROWS)), 0.0)
            kaug[h, pl.ds(at, ROWS), 128:] = tail.T.astype(bf16)
        vt[:, pl.ds(at, ROWS)] = kv[i][:ROWS, 128:].astype(f32).T.astype(bf16)


def attn_kernel(steps, nz, zy, *refs):
    n = len(steps)
    qrefs, kaug, vt = refs[:n], refs[n], refs[n + 1]
    outs = refs[n + 2 : 2 * n + 2]
    qa, r, s, after = refs[2 * n + 2 :]
    after[...] = jnp.where(
        lax.broadcasted_iota(jnp.int32, (KT, KT), 1) > lax.broadcasted_iota(jnp.int32, (KT, KT), 0), -1.0, 0.0
    ).astype(bf16)

    def tiles(js, own):
        units = [(j, h, q) for j in js for q in range(ROWS // QC) for h in range(2)]
        n = len(units)
        carry = {(h, q): s[8 * h : 8 * h + 1, q * QC : q * QC + QC] for h in range(2) for q in range(ROWS // QC)}
        zs, takes, sums, sps, outs_ = {}, {}, {}, {}, {}

        def score(u):
            j, h, q = units[u]
            at = pl.multiple_of(j * KT, KT)
            zs[u] = jnp.dot(kaug[h, pl.ds(at, KT), :], qa[h, :, q * QC : q * QC + QC], preferred_element_type=f32)

        def soft(u):
            j, h, q = units[u]
            z = zs.pop(u)
            sp = jnp.maximum(z, lax.log2(1.0 + jnp.exp2(jnp.minimum(z, 126.0))))
            take = z - sp
            if own is not None:
                ok = (
                    lax.broadcasted_iota(jnp.int32, (KT, QC), 0) + own * KT
                    < lax.broadcasted_iota(jnp.int32, (KT, QC), 1) + q * QC
                )
                sp = jnp.where(ok, sp, 0.0)
                take = jnp.where(ok, take, -1e30)
            takes[u], sps[u] = take, sp[0:1, :]
            sums[u] = jnp.dot(after[...], sp.astype(bf16), preferred_element_type=f32)

        def weigh(u):
            j, h, q = units[u]
            at = pl.multiple_of(j * KT, KT)
            a = sums.pop(u)
            w = jnp.exp2(takes.pop(u) + a).astype(bf16)
            outs_[u] = (
                jnp.dot(vt[64 * h : 64 * h + 64, pl.ds(at, KT)], w, preferred_element_type=f32),
                jnp.exp2(carry[h, q]),
            )
            carry[h, q] = carry[h, q] + (a[0:1, :] - sps.pop(u))

        def add(u):
            j, h, q = units[u]
            o, scale = outs_.pop(u)
            r[64 * h : 64 * h + 64, q * QC : q * QC + QC] += scale * o

        stages = (score, soft, weigh, add)
        lags = (0, L1, L1 + L2, L1 + L2 + L3)
        for t in range(n + lags[-1]):
            for stage, lag in zip(stages, lags):
                if 0 <= t - lag < n:
                    stage(t - lag)
        for (h, q), value in carry.items():
            s[8 * h : 8 * h + 1, q * QC : q * QC + QC] = value

    c = bf16_parts(LOG2E, 3)
    row = lax.broadcasted_iota(jnp.int32, (128, ROWS), 0)
    tail = jnp.where(row == 0, c[0], jnp.where(row == 1, c[1], jnp.where(row == 2, c[2], 0.0))).astype(bf16)

    def load(qref):
        q = (qref[...].astype(f32) * (LOG2E / 8)).T
        hi = q.astype(bf16).astype(f32)
        lo = q - hi
        for h in range(2):
            mine = slice(64 * h, 64 * h + 64)
            qa[h, :64, :] = hi[mine].astype(bf16)
            qa[h, 64:128, :] = lo[mine].astype(bf16)
            qa[h, 128:, :] = tail
        r[...] = jnp.zeros_like(r)
        s[...] = jnp.zeros_like(s)

    def store(out):
        out[:128, :] = r[...].astype(bf16)
        rows16 = lax.broadcasted_iota(jnp.int32, (16, ROWS), 0)
        block = jnp.zeros((16, ROWS), f32)
        for h in range(2):
            line = s[8 * h : 8 * h + 1, :]
            big = line.astype(bf16).astype(f32)
            for p, part in enumerate((big, line - big)):
                block = jnp.where(rows16 == h * 2 + p, jnp.broadcast_to(part, (16, ROWS)), block)
        out[128:, :] = block.astype(bf16)

    if steps == (0,):
        load(qrefs[0])
        y = zy[YAT]

        @pl.loop(0, 2)
        def _(m):
            tiles([2 * y + 1 - m], 1 - m)

        @pl.loop(0, y)
        def _(m):
            tiles([2 * (y - 1 - m) + 1, 2 * (y - 1 - m)], None)

        store(outs[0])
        return

    @pl.loop(0, n)
    def _(i):
        far = steps[0] - i

        @pl.when(zy[ZAT] + far <= nz - 1)
        def _():
            for m in range(n):
                pl.when(i == m)(functools.partial(load, qrefs[m]))

            @pl.loop(0, 8 // UN)
            def _(m):
                tiles([7 - UN * m - u for u in range(UN)], None)

            for m in range(n):
                pl.when(i == m)(functools.partial(store, outs[m]))


def combine_kernel(nk, gain, conv, *refs):
    payloads, out = refs[:nk], refs[nk:]
    heads = []
    for h in range(2):
        mine = slice(64 * h, 64 * h + 64)
        total = payloads[0][mine, :].astype(f32)
        s = jnp.zeros((1, ROWS), f32)
        for k in range(1, nk):
            b = payloads[k - 1][128:, :].astype(f32)
            s = s + b[2 * h : 2 * h + 1] + b[2 * h + 1 : 2 * h + 2]
            total = total + jnp.exp2(s) * payloads[k][mine, :].astype(f32)
        mean = jnp.sum(total * total, axis=0, keepdims=True) * (1.0 / 64)
        heads.append(total * lax.rsqrt(mean + 1e-6))
    res = (jnp.concatenate(heads, axis=0).T * gain[...]).astype(bf16)
    for half in range(2):
        rows = slice(256 * half, 256 * half + 256)
        out[half][:, :128] = res[rows]
        out[half][:, 128:] = conv[rows, :]


VM = pl.BlockSpec(memory_space=pltpu.VMEM)
SM = pl.BlockSpec(memory_space=pltpu.SMEM)
HB = pl.BlockSpec(memory_space=pltpu.HBM)
PARAMS = pltpu.CompilerParams(vmem_limit_bytes=48 * 1024 * 1024)


def prep(zy, kvs):
    return pl.pallas_call(
        prep_kernel,
        out_shape=(jax.ShapeDtypeStruct((2, 2048, 256), bf16), jax.ShapeDtypeStruct((128, 2048), bf16)),
        in_specs=[SM] + [VM] * 4,
        out_specs=(VM, VM),
        compiler_params=PARAMS,
        name="prep",
    )(zy, *kvs)


def attend(steps, nz, zy, qs, kaug, vt):
    n = len(steps)
    cost = pl.CostEstimate(flops=2 * n * ROWS * 2048 * 256 * 6, bytes_accessed=4 * 2**20, transcendentals=3 * n * ROWS * 2048 * 2)
    return pl.pallas_call(
        functools.partial(attn_kernel, steps, nz),
        out_shape=tuple(jax.ShapeDtypeStruct((144, ROWS), bf16) for _ in steps),
        in_specs=[SM] + [VM] * (n + 2),
        out_specs=tuple(VM for _ in steps),
        scratch_shapes=[
            pltpu.VMEM((2, 256, ROWS), bf16),
            pltpu.VMEM((128, ROWS), f32),
            pltpu.VMEM((16, ROWS), f32),
            pltpu.VMEM((KT, KT), bf16),
        ],
        cost_estimate=cost,
        compiler_params=PARAMS,
        name="attend_" + "_".join(map(str, steps)),
    )(zy, *qs, kaug, vt)


def combine(gain, conv, payloads):
    n = len(payloads)
    return pl.pallas_call(
        functools.partial(combine_kernel, n),
        out_shape=(jax.ShapeDtypeStruct((256, 256), bf16),) * 2,
        in_specs=[VM] * (n + 2),
        out_specs=(VM, VM),
        compiler_params=PARAMS,
        name="combine",
    )(gain, conv, *payloads)


def project_kernel(shape, base, first, last, info, gains, *refs):
    count = len(shape)
    parts = []
    for n in shape:
        parts.append(refs[:n])
        refs = refs[n:]
    weights, refs = refs[:6], refs[6:]
    wbuf, sems = refs[-2:]
    refs = refs[:-2]
    copies = [
        pltpu.make_async_copy(
            w.at[pl.ds(pl.multiple_of(info[base + i] * 512, 512), 512), :],
            wbuf.at[pl.ds(512 * i, 512), pl.ds(128 * j, 128)],
            sems.at[i, j],
        )
        for i in range(count)
        for j, w in enumerate(weights)
    ]
    for copy in copies:
        copy.start()
    if not first:
        before, refs = refs[:2], refs[2:]
    if last:
        bias, q_out, kv_out, gate_out = refs
    acc = ssq = None
    for p in range(count // 2):
        xs = []
        for i in range(2 * p, 2 * p + 2):
            pieces = [piece[...] for piece in parts[i]]
            x = (pieces[0] if len(pieces) == 1 else jnp.concatenate(pieces, axis=0)).astype(f32)
            xx = x * x
            sq = (xx[:, :128] + xx[:, 128:256]) + (xx[:, 256:384] + xx[:, 384:])
            ssq = sq if ssq is None else ssq + sq
            xs.append((x * gains[info[base + i]]).astype(bf16))
        for copy in copies[12 * p : 12 * p + 12]:
            copy.wait()
        add = jnp.dot(jnp.concatenate(xs, axis=1), wbuf[1024 * p : 1024 * p + 1024, :], preferred_element_type=f32)
        acc = add if acc is None else acc + add
    if not first:
        acc = acc + before[0][...]
        ssq = ssq + before[1][...]
    if not last:
        refs[0][...] = acc
        refs[1][...] = ssq
        return
    mean = jnp.sum(ssq, axis=1, keepdims=True) * (1.0 / FEATURES)
    res = (acc * lax.rsqrt(mean + EPS)).astype(bf16)
    q_out[...] = res[:, :128]
    kv_out[:ROWS, :] = res[:, 128:384]
    gate_out[...] = res[:, 384:]
    wide = jnp.concatenate([bias[...].astype(f32), jnp.zeros((ROWS, 126), f32)], axis=1).T
    rows16 = lax.broadcasted_iota(jnp.int32, (16, 256), 0)
    block = jnp.zeros((16, 256), f32)
    for h in range(2):
        for t in range(2):
            piece = jnp.broadcast_to(wide[h : h + 1, 256 * t : 256 * t + 256], (16, 256))
            block = jnp.where(rows16 == 2 * h + t, piece, block)
    kv_out[ROWS:, :] = block.astype(bf16)


def project(info, base, parts, gains, weights, before, bias):
    shape = tuple(len(part) for part in parts)
    count = len(parts)
    extra = () if before is None else before
    shapes = (jax.ShapeDtypeStruct((ROWS, 768), f32), jax.ShapeDtypeStruct((ROWS, 128), f32))
    if bias is not None:
        extra = (*extra, bias)
        shapes = tuple(jax.ShapeDtypeStruct(s, bf16) for s in ((ROWS, 128), (ROWS + 16, 256), (ROWS, 384)))
    flat = [array for part in parts for array in part]
    return pl.pallas_call(
        functools.partial(project_kernel, shape, base, before is None, bias is not None),
        in_specs=[SM, VM] + [VM] * len(flat) + [HB] * 6 + [VM] * len(extra),
        out_specs=tuple(VM for _ in shapes),
        out_shape=shapes,
        scratch_shapes=[pltpu.VMEM((512 * count, 768), bf16), pltpu.SemaphoreType.DMA((count, 6))],
        cost_estimate=pl.CostEstimate(flops=2 * count * 512 * 512 * 768, bytes_accessed=count * 2**20, transcendentals=0),
        compiler_params=PARAMS,
        name="project_%d" % count,
    )(info, gains, *flat, *weights, *extra)


def conv_kernel(gates, before, taps, gain, out):
    mixed = gates[:, 128:256].astype(f32) * gates[:, 256:].astype(f32)
    old = before[:, :128].astype(f32) * before[:, 128:].astype(f32)
    row = lax.broadcasted_iota(jnp.int32, (ROWS, 128), 0)
    prev = lambda i: jnp.broadcast_to(old[i : i + 1], (ROWS, 128))
    one = jnp.where(row == 0, prev(1), pltpu.roll(mixed, 1, 0))
    two = jnp.where(row == 0, prev(0), jnp.where(row == 1, prev(1), pltpu.roll(mixed, 2, 0)))
    conv = taps[0:1] * two + taps[1:2] * one + taps[2:3] * mixed
    conv = gates[:, :128].astype(f32) * conv
    low = lax.broadcasted_iota(jnp.int32, (ROWS, 128), 1) < 64
    sq = conv * conv
    m0 = jnp.sum(jnp.where(low, sq, 0.0), axis=1, keepdims=True)
    m1 = jnp.sum(jnp.where(low, 0.0, sq), axis=1, keepdims=True)
    mean = jnp.where(low, m0, m1) * (1.0 / HEAD)
    out[...] = (conv * lax.rsqrt(mean + EPS) * gain[...]).astype(bf16)


def convolve(gates, before, taps, gain):
    return pl.pallas_call(
        conv_kernel,
        out_shape=jax.ShapeDtypeStruct((ROWS, 128), bf16),
        in_specs=[VM] * 4,
        out_specs=VM,
        compiler_params=PARAMS,
        name="convolve",
    )(gates, before, taps, gain)


def regroup_kernel(info, attn, conv, *refs):
    outs, sems = refs[:4], refs[4]
    copies = []
    for j, by in enumerate((0, 1, 3, 2)):
        at = pl.multiple_of(lax.rem(info[CHIP] + by, 4) * 1024, 1024)
        for i, w in enumerate((attn, conv)):
            copies.append(
                pltpu.make_async_copy(w.at[:, pl.ds(at, 1024)], outs[j].at[pl.ds(128 * i, 128), :], sems.at[j, i])
            )
    for copy in copies:
        copy.start()
    for copy in copies:
        copy.wait()


def regroup(info, out_attn, out_conv):
    return pl.pallas_call(
        regroup_kernel,
        in_specs=[SM, HB, HB],
        out_specs=(HB,) * 4,
        out_shape=(jax.ShapeDtypeStruct((256, 1024), bf16),) * 4,
        scratch_shapes=[pltpu.SemaphoreType.DMA((4, 2))],
        compiler_params=PARAMS,
        name="regroup",
    )(info, out_attn, out_conv)


def output_kernel(mine, info, *refs):
    w, parts, out = refs[:4], refs[4:12], refs[12]
    core = info[CORE] if mine else 1 - info[CORE]
    at = pl.multiple_of(core * 512, 512)
    total = jnp.zeros((ROWS, 512), f32)
    for i in range(4):
        x = jnp.concatenate([parts[2 * i][...], parts[2 * i + 1][...]], axis=0)
        total = total + jnp.dot(x, w[i][:, pl.ds(at, 512)], preferred_element_type=f32)
    out[...] = total.astype(out.dtype)


def output(mine, info, w, parts):
    return pl.pallas_call(
        functools.partial(output_kernel, mine),
        in_specs=[SM] + [VM] * 12,
        out_specs=VM,
        out_shape=jax.ShapeDtypeStruct((ROWS, 512), f32 if mine else bf16),
        cost_estimate=pl.CostEstimate(flops=2 * 512 * 1024 * 512, bytes_accessed=3 * 2**20, transcendentals=0),
        compiler_params=PARAMS,
        name="output_mine" if mine else "output_other",
    )(info, *w, *parts)


def along_x(shard, by):
    return lax.ppermute(shard, "tp", [(i, (i + 2 * by) % 8) for i in range(8)])


def other_core(shard):
    return lax.ppermute(shard, "tp", [(i, i ^ 1) for i in range(8)])


def along_y(shard, by):
    count = lax.axis_size("sp")
    return lax.ppermute(shard, "sp", [(i, i // NY * NY + (i + by) % NY) for i in range(count)])


def along_z(shard, by):
    count = lax.axis_size("sp")
    return lax.ppermute(shard, "sp", [(i, i + NY * by) for i in range(count) if 0 <= i + NY * by < count])


def per_device(
    tokens,
    norm_gain,
    w_query,
    w_key,
    w_value,
    w_gate_out,
    w_gate_in,
    w_conv_in,
    conv_taps,
    key_bias,
    mix_gain,
    out_attn,
    out_conv,
):
    cols = w_query.shape[1]
    t = lax.axis_index("tp")
    sp_index = lax.axis_index("sp")
    count = lax.axis_size("sp")
    nz = count // NY
    weights = (w_query, w_key, w_value, w_gate_out, w_gate_in, w_conv_in)
    gains = norm_gain.reshape(8, 1, 512)
    order = [(0, 0), (0, 1), (6, 0), (6, 1), (2, 0), (2, 1), (4, 0), (4, 1)]
    table = np.zeros((count * 8, 16), np.int32)
    for at in range(count * 8):
        sp, tp = divmod(at, 8)
        table[at, :12] = [((tp ^ c) + by) % 8 for by, c in order] + [tp // 2, tp % 2, sp // NY, sp % NY]
    info = lax.dynamic_slice(jnp.asarray(table), (sp_index * 8 + t, 0), (1, 16))[0]

    top, bottom = tokens[:256], tokens[256:]
    a_top, b_bottom = along_x(top, 1), along_x(bottom, -1)
    tokens_s = other_core(tokens)
    a_bottom, b_top = along_x(bottom, 1), along_x(top, -1)
    state = project(info, 0, [[tokens], [tokens_s]], gains, weights, None, None)
    a_top, b_bottom, *state = lax.optimization_barrier((a_top, b_bottom, *state))
    far_top, far_bottom = along_x(a_top, 1), along_x(b_bottom, -1)
    pair = lambda x, y: [[x, y], [other_core(x), other_core(y)]]
    state = project(info, 2, pair(a_top, a_bottom) + pair(b_top, b_bottom), gains, weights, tuple(state), None)
    blocks = regroup(info, out_attn, out_conv)
    far_top, *blocks = lax.optimization_barrier((far_top, *blocks))
    queries, keys_values, gates = project(info, 6, pair(far_top, far_bottom), gains, weights, tuple(state), key_bias)
    out_cols = [blocks[0], along_x(blocks[1], 1), along_x(blocks[2], -1), along_x(blocks[3], 2)]

    kvs = [keys_values] + [along_y(keys_values, k) for k in range(1, NY)]
    qs = [queries] + [along_z(queries, -k) for k in range(1, nz)]
    before = lax.ppermute(gates[ROWS - CONV_WIDTH + 1 :, cols:], "sp", [(i, i + 1) for i in range(count - 1)])
    taps = lax.dynamic_slice_in_dim(conv_taps, t * cols, cols, 1)
    attn_gain = lax.dynamic_slice_in_dim(mix_gain, t * cols, cols)
    conv_gain = lax.dynamic_slice_in_dim(mix_gain, STICK_HEADS * HEAD + t * cols, cols)
    conv_normed = convolve(gates, before, taps, conv_gain[None])

    kaug, vt = prep(info, kvs)
    payloads = [None] * nz
    for steps in GROUPS:
        for k, mine in zip(steps, attend(steps, nz, info, [qs[k] for k in steps], kaug, vt)):
            payloads[k] = along_z(mine, k) if k else mine
    top, bottom = combine(attn_gain[None], conv_normed, payloads)
    a_top, b_bottom = along_x(top, 1), along_x(bottom, -1)
    a_bottom, b_top = along_x(bottom, 1), along_x(top, -1)
    far_top, far_bottom = along_x(a_top, 1), along_x(b_bottom, -1)
    parts = (top, bottom, a_top, a_bottom, b_top, b_bottom, far_top, far_bottom)
    received = other_core(output(False, info, out_cols, parts))
    own = output(True, info, out_cols, parts)
    return (own + received.astype(f32)).astype(bf16)


def solution(mesh):
    in_specs = (
        P("sp", "tp"),
        P(),
        P(None, "tp"),
        P(None, "tp"),
        P(None, "tp"),
        P(None, "tp"),
        P(None, "tp"),
        P(None, "tp"),
        P(),
        P("sp", "tp"),
        P(),
        P("tp", None),
        P("tp", None),
    )
    return jax.shard_map(
        per_device, mesh=mesh, in_specs=in_specs, out_specs=P("sp", "tp"), check_vma=False
    )
```
